32 devices in a mesh: sp: 8 (over z, y), tp: 4 (over x, core).
Axes of the slice: x: 2, y: 2, z: 4, core: 2. Of those that a mesh axis runs over, the one named last changes fastest.
Arguments:
- query: bfloat16 [2048, 1536], P('sp', 'tp'), may hold values from -6 to 6
- forget_preact: bfloat16 [2048, 1536], P('sp', 'tp'), may hold values from -6 to 6
- value_input: bfloat16 [2048, 1536], P('sp', 'tp'), may hold values from -6 to 6
- output_gate: bfloat16 [2048, 1536], P('sp', 'tp'), may hold values from -6 to 6
- forget_minimum: float32 [1536], P('tp'), may hold values from 0.88 to 1
- extra_log_decay: float32 [12, 2048], P('tp', 'sp'), may hold values from -0.7 to 0
- head_norm_gain: float32 [1536], P('tp'), may hold values from 0.1 to 1.9
- output_weight: bfloat16 [1536, 3072], P(None, 'tp'), may hold values from -0.15625 to 0.15625
- stream: bfloat16 [2048, 3072], P(('sp', 'tp')), may hold values from -6 to 6
- feedforward_gain: float32 [3072], replicated, may hold values from 0.1 to 1.9
- routes: int32 [2048, 2], P('sp'), may hold values from 0 to 7, all different within a row; in each aligned block of 64 rows (0 to 63, 64 to 127, ...) at most 32 rows name the same one
- router_weight: float32 [2048, 2], P(('sp', 'tp')), may hold values from 0.05 to 1
- expert_gate_weight: bfloat16 [8, 3072, 1024], P('sp', None, 'tp'), may hold values from -0.109375 to 0.109375
- expert_up_weight: bfloat16 [8, 3072, 1024], P('sp', None, 'tp'), may hold values from -0.109375 to 0.109375
- expert_down_weight: bfloat16 [8, 1024, 3072], P('sp', 'tp'), may hold values from -0.1875 to 0.1875
Outputs:
- result: bfloat16 [2048, 3072], P(('sp', 'tp'))
The draws below stay inside these ranges and needn't reach their ends.
Inputs may be any that keep to these rules, and one draw needn't show every extreme that they name: `routes`: each row names 2 different experts; in each aligned block of 64 rows no expert is named by more than 32 rows, a bound that some block reaches.
All inputs are finite; a program needn't handle non-finite values.
Results may differ from the reference program's by a relative error of at most 0.01.
Values may be sent and summed in bfloat16 or wider, within the bound.
A program may use at most 64 MiB of HBM per device.

```python
import math
import jax
import jax.numpy as jnp
import numpy as np
from jax import lax

D = 3072
HEADS = 12
STATE_ROW_COUNT = 128
VALUE_CHANNELS = 128
FF = 1024
SPAN = 64
TOPK = 2
TOK_DEV = 256
SEQUENCE_TOKENS = 2048
KEY_WIDTH = 1536
VALUE_WIDTH = 1536
EXPERTS = 8
QROWS = 64
CAPQ = 32
N_TP = 4


def draw_forget_preact(key, part):
    base_key, shift_key = jax.random.split(key)
    base_draw = jax.random.normal(base_key, (SEQUENCE_TOKENS, KEY_WIDTH), jnp.float32)
    shift_draw = jax.random.uniform(shift_key, (SEQUENCE_TOKENS // TOK_DEV, 1), jnp.float32, -1.0, 1.0)
    shifted = base_draw + jnp.repeat(shift_draw, TOK_DEV, axis=0)
    return jnp.clip(shifted, -6.0, 6.0).astype(jnp.bfloat16)


def draw_forget_minimum(key, part):
    pick_key, slow_key, fast_key = jax.random.split(key, 3)
    slow_share = 0.5
    slow_head = jax.random.uniform(pick_key, (HEADS, 1), jnp.float32) < slow_share
    slow_rate = jnp.exp(jax.random.uniform(slow_key, (HEADS, STATE_ROW_COUNT), jnp.float32, jnp.log(0.2), jnp.log(2.0))) / SEQUENCE_TOKENS
    fast_rate = jnp.exp(jax.random.uniform(fast_key, (HEADS, STATE_ROW_COUNT), jnp.float32, jnp.log(0.04), jnp.log(0.12)))
    decay_rate = jnp.where(slow_head, slow_rate, fast_rate)
    return (1.0 - decay_rate).reshape(HEADS * STATE_ROW_COUNT).astype(jnp.float32)


def draw_extra_log_decay(key, part):
    location_seed, size_key = jax.random.split(key)
    spike_places = jax.random.randint(location_seed, (4,), 0, SEQUENCE_TOKENS)
    spike_mask = jnp.any(jnp.arange(SEQUENCE_TOKENS)[None, :] == spike_places[:, None], axis=0)
    retained_fraction = jax.random.uniform(size_key, (HEADS, 1), jnp.float32, 0.5, 0.8)
    return jnp.where(spike_mask[None, :], jnp.log(retained_fraction), 0.0).astype(jnp.float32)


def level_of(rng, dims, shards, least, largest):
    level = 1.0
    for dim, blocks in shards:
        heights = jax.random.uniform(jax.random.fold_in(jax.random.fold_in(rng, 6), dim), (blocks,), jnp.float32, least / len(shards), largest / len(shards))
        level = level * jnp.repeat(jnp.exp(heights), dims[dim] // blocks).reshape((-1,) + (1,) * (len(dims) - 1 - dim))
    return level


def assign_block(key, own, number, rows, number_of, top, reach, skew):
    ranking = jax.random.permutation(key, number_of)
    heavy_load, ordinary = portions_of(number_of, rows * top, reach, skew, True), portions_of(number_of, rows * top, reach, skew, False)
    places = jnp.arange(number_of)

    def named(tallies, rotation):
        used = int((tallies > 0).sum())
        fixed = max(1, used // 4)
        passed = fixed + (places - fixed + rotation * (used - fixed)) % max(1, number_of - fixed)
        return jnp.zeros((number_of,), jnp.int32).at[ranking[jnp.where(places < fixed, places, passed)]].set(jnp.asarray(tallies, jnp.int32))

    tallies = jnp.where(number % 4 == 0, named(heavy_load, number // 4), named(ordinary, number - number // 4 - 1))
    mixed = jax.random.permutation(jax.random.fold_in(own, 3), number_of)
    giver, taker = mixed[0:number_of // 2 * 2:2], mixed[1:number_of // 2 * 2:2]
    slack = jnp.minimum(tallies[giver] - 1, reach - tallies[taker]) // 2
    slack = jnp.where((giver == ranking[0]) | (taker == ranking[0]) | (tallies[taker] == 0), 0, jnp.maximum(slack, 0))
    passed = jax.random.randint(jax.random.fold_in(own, 4), (number_of // 2,), 0, 1 << 20) % (slack + 1)
    tallies = tallies.at[giver].add(-passed).at[taker].add(passed)
    members = jnp.searchsorted(jnp.cumsum(tallies), jnp.arange(rows * top), side="right").astype(jnp.int32)
    listing = members.reshape(top, rows).T
    listing = listing[jax.random.permutation(jax.random.fold_in(own, 1), rows)]
    rotation = jax.random.randint(jax.random.fold_in(own, 2), (rows, 1), 0, top)
    return jnp.take_along_axis(listing, (jnp.arange(top)[None, :] + rotation) % top, axis=1)


def portions_of(number_of, total, bound, lean, full):
    portions = [(1 << 20) // math.isqrt(standing ** lean) + 1 for standing in range(1, number_of + 1)]
    largest = bound if full else min(bound, max(-(-total // number_of), total * portions[0] // sum(portions)))
    least = 1 if total - largest >= number_of - 1 else 0
    holding, rest = [largest] + [least] * (number_of - 1), total - largest - least * (number_of - 1)
    while rest > 0:
        candidates = [i for i in range(1, number_of) if holding[i] < largest] or [i for i in range(1, number_of) if holding[i] < bound]
        pool, budget = sum([portions[i] for i in candidates]), rest
        for i in candidates:
            addition = min(bound - holding[i], max(1, budget * portions[i] // pool), rest)
            holding[i] = holding[i] + addition
            rest = rest - addition
    return np.array(holding)


def noise(rng, dims, scale, limit, pieces=(), kind=jnp.bfloat16):
    loudness = level_of(rng, dims, pieces, -0.22, 0.18) if pieces else 1.0
    values = jax.random.normal(rng, dims, jnp.float32) * scale * loudness
    return jnp.minimum(jnp.maximum(values, -limit), limit).astype(kind)


def setup_inputs(seed: int = 0) -> dict:
    streams_of = jax.random.split(jax.random.key(seed), 16)
    query = noise(streams_of[0], (SEQUENCE_TOKENS, KEY_WIDTH), 1.0, 6.0, ((0, 8), (1, 4)))
    forget_preact = draw_forget_preact(jax.random.fold_in(streams_of[15], 71), 0)
    value_input = noise(streams_of[2], (SEQUENCE_TOKENS, VALUE_WIDTH), 1.0, 6.0, ((0, 8), (1, 4)))
    output_gate = noise(streams_of[3], (SEQUENCE_TOKENS, VALUE_WIDTH), 1.0, 6.0, ((0, 8), (1, 4)))
    forget_minimum = draw_forget_minimum(jax.random.fold_in(streams_of[15], 71), 0)
    extra_log_decay = draw_extra_log_decay(jax.random.fold_in(streams_of[15], 71), 0)
    head_norm_gain = jnp.clip(1.0 + 0.18 * jax.random.normal(streams_of[6], (VALUE_WIDTH,), jnp.float32), 0.1, 1.9)
    output_weight = noise(streams_of[7], (VALUE_WIDTH, D), VALUE_WIDTH ** -0.5, 0.15625, ((1, 4),))
    stream = noise(streams_of[8], (SEQUENCE_TOKENS, D), 1.0, 6.0, ((0, 32),))
    feedforward_gain = jnp.clip(1.0 + 0.18 * jax.random.normal(streams_of[9], (D,), jnp.float32), 0.1, 1.9)
    routes_keys = jax.random.split(jax.random.fold_in(streams_of[10], 1), SEQUENCE_TOKENS // QROWS)
    routes_turns = jax.random.permutation(jax.random.fold_in(streams_of[10], 3), SEQUENCE_TOKENS // QROWS)
    routes = jax.vmap(lambda own, number: assign_block(jax.random.fold_in(streams_of[10], 2), own, number, QROWS, EXPERTS, TOPK, CAPQ, 2))(routes_keys, routes_turns).reshape((SEQUENCE_TOKENS, TOPK))
    router_weight = jnp.clip(0.05 + 0.95 * jax.random.uniform(streams_of[11], (SEQUENCE_TOKENS, TOPK), jnp.float32) ** level_of(streams_of[11], (SEQUENCE_TOKENS, TOPK), ((0, 32),), -0.2, 0.2), 0.05, 1.0)
    expert_gate_weight = noise(streams_of[12], (EXPERTS, D, FF), D ** -0.5, 0.109375, ((0, 8), (2, 4)))
    expert_up_weight = noise(streams_of[13], (EXPERTS, D, FF), D ** -0.5, 0.109375, ((0, 8), (2, 4)))
    expert_down_weight = noise(streams_of[14], (EXPERTS, FF, D), FF ** -0.5, 0.1875, ((0, 8), (1, 4)))
    return dict(query=query, forget_preact=forget_preact, value_input=value_input, output_gate=output_gate, forget_minimum=forget_minimum, extra_log_decay=extra_log_decay, head_norm_gain=head_norm_gain, output_weight=output_weight, stream=stream, feedforward_gain=feedforward_gain, routes=routes, router_weight=router_weight, expert_gate_weight=expert_gate_weight, expert_up_weight=expert_up_weight, expert_down_weight=expert_down_weight)


epsilon = 1e-06
top_precision = lax.Precision.HIGHEST
tile_rows = 256

def block_step(current_state, block_inputs):
    query_block, weight_blk, value_block, decay_blk = block_inputs
    running_decay = jnp.cumsum(decay_blk, axis=1)
    intermediate = jnp.einsum('yro,yow->yrw', query_block * jnp.exp(running_decay), current_state, precision=top_precision)
    causal = lax.broadcasted_iota(jnp.int32, (SPAN, SPAN), 0) >= lax.broadcasted_iota(jnp.int32, (SPAN, SPAN), 1)
    log_gap = running_decay[:, :, None, :] - running_decay[:, None, :, :]
    decay_table = jnp.exp(jnp.where(causal[None, :, :, None], log_gap, -jnp.inf))
    scores = jnp.einsum('htk,hsk,htsk->hts', query_block, weight_blk, decay_table, precision=top_precision)
    output = intermediate + jnp.einsum('hts,hsv->htv', scores, value_block, precision=top_precision)
    final_decay = running_decay[:, -1:, :]
    scaled_rows = weight_blk * jnp.exp(final_decay - running_decay)
    following_state = jnp.exp(final_decay[:, 0, :])[:, :, None] * current_state + jnp.einsum('xme,xmc->xec', scaled_rows, value_block, precision=top_precision)
    return (following_state, output)

def gate_factors(query, forget_preact, forget_minimum, extra_log_decay):
    query_activated = jax.nn.silu(query.astype(jnp.float32))
    incoming_weight = (1.0 - forget_minimum) * jax.nn.sigmoid(-forget_preact.astype(jnp.float32))
    spike_columns = jnp.repeat(jnp.transpose(extra_log_decay), STATE_ROW_COUNT, axis=1)
    decay_logarithm = jnp.log1p(-incoming_weight) + spike_columns
    return (query_activated, incoming_weight, decay_logarithm)

def head_blocks(array_in, head_total):
    rows_in = array_in.shape[0]
    return array_in.reshape(rows_in // SPAN, SPAN, head_total, -1).transpose(0, 2, 1, 3)

def head_output(mixed, head_norm_gain, output_gate):
    normalized = mixed * lax.rsqrt(lax.optimization_barrier(jnp.mean(mixed * mixed, axis=-1, keepdims=True)) + epsilon)
    flat_rows = normalized.reshape(mixed.shape[0], -1)
    return (flat_rows * head_norm_gain * jax.nn.silu(output_gate.astype(jnp.float32))).astype(jnp.bfloat16)

def rms_norm(residual, gain):
    scale_row = lax.rsqrt(lax.optimization_barrier(jnp.mean(residual * residual, axis=-1, keepdims=True)) + epsilon)
    return (residual * scale_row * gain).astype(jnp.bfloat16)

def expert_rows(row_data, gate_w, up_w, down_w):
    gate_act = jnp.dot(row_data, gate_w, preferred_element_type=jnp.float32)
    up_act = jnp.dot(row_data, up_w, preferred_element_type=jnp.float32)
    inner_act = (jax.nn.silu(gate_act) * up_act).astype(jnp.bfloat16)
    quarter = inner_act.shape[1] // N_TP
    parts = jnp.einsum('njf,jfd->njd', inner_act.reshape(-1, N_TP, quarter).astype(jnp.float32), down_w.reshape(N_TP, quarter, -1).astype(jnp.float32))
    parts = lax.optimization_barrier(parts.astype(jnp.bfloat16))
    return lax.optimization_barrier(jnp.sum(parts.astype(jnp.float32), axis=1)).astype(jnp.bfloat16)

def routed(normed, routes, route_weight, expert_gate_weight, expert_up_weight, expert_down_weight):
    pick_ids = routes.reshape(-1).astype(jnp.int32)
    flat_weight = route_weight.reshape(-1)
    expert_ids = jnp.arange(EXPERTS, dtype=jnp.int32)
    counts = lax.optimization_barrier(jnp.sum((pick_ids[:, None] == expert_ids[None, :]).astype(jnp.int32), axis=0)).astype(jnp.int32)
    starts = (jnp.cumsum(counts) - counts).astype(jnp.int32)
    sort_order = jnp.argsort(pick_ids, stable=True).astype(jnp.int32)
    padded = jnp.concatenate([sort_order, jnp.zeros((tile_rows,), jnp.int32)])
    result = jnp.zeros((normed.shape[0], normed.shape[1]), jnp.float32)

    def per_expert(expert_id, result_now):
        tile_count = ((counts[expert_id] + tile_rows - 1) // tile_rows).astype(jnp.int32)

        def per_tile(tile_id, result_tile):
            offset = (tile_id * tile_rows).astype(jnp.int32)
            row_ids = lax.dynamic_slice_in_dim(padded, (starts[expert_id] + offset).astype(jnp.int32), tile_rows)
            valid_rows = offset + jnp.arange(tile_rows, dtype=jnp.int32) < counts[expert_id]
            row_data = normed[row_ids // TOPK]
            output = expert_rows(row_data, expert_gate_weight[expert_id], expert_up_weight[expert_id], expert_down_weight[expert_id])
            weighted = jnp.where(valid_rows, flat_weight[row_ids], 0.0)[:, None] * output.astype(jnp.float32)
            return result_tile.at[row_ids // TOPK].add(weighted)
        return lax.fori_loop(jnp.int32(0), tile_count, per_tile, result_now)
    return lax.fori_loop(0, EXPERTS, per_expert, result)

def reference(query, forget_preact, value_input, output_gate, forget_minimum, extra_log_decay, head_norm_gain, output_weight, stream, feedforward_gain, routes, router_weight, expert_gate_weight, expert_up_weight, expert_down_weight):
    query_activated, incoming_weight, decay_logarithm = gate_factors(query, forget_preact, forget_minimum, extra_log_decay)
    value_rows = value_input.astype(jnp.float32)
    blocks = (head_blocks(query_activated, HEADS), head_blocks(incoming_weight, HEADS), head_blocks(value_rows, HEADS), head_blocks(decay_logarithm, HEADS))
    start_state = jnp.zeros((HEADS, STATE_ROW_COUNT, VALUE_CHANNELS), jnp.float32)
    _, block_outs = lax.scan(block_step, start_state, blocks)
    mixed = block_outs.transpose(0, 2, 1, 3).reshape(SEQUENCE_TOKENS, HEADS, VALUE_CHANNELS)
    hidden = head_output(mixed, head_norm_gain, output_gate)
    mix_rows = jnp.dot(hidden, output_weight, preferred_element_type=jnp.float32).astype(jnp.bfloat16)
    mix_rows = lax.optimization_barrier(mix_rows)
    residual = stream.astype(jnp.float32) + mix_rows.astype(jnp.float32)
    normed = rms_norm(residual, feedforward_gain)
    route_weight = router_weight / lax.optimization_barrier(jnp.sum(router_weight, axis=1, keepdims=True))
    routed_sum = routed(normed, routes, route_weight, expert_gate_weight, expert_up_weight, expert_down_weight)
    return (residual + routed_sum).astype(jnp.bfloat16)
```

```python
import functools

import jax
import jax.numpy as jnp
from jax import lax
from jax.experimental import pallas as pl
from jax.experimental.pallas import tpu as pltpu
from jax.sharding import PartitionSpec as P

STATE_ROW_COUNT = 128
VALUE_CHANNELS = 128
SPAN = 64
TOPK = 2


epsilon = 1e-06
MESH = pl.DeviceIdType.MESH


def silu(x):
    return x / (1.0 + jnp.exp(-x))


def nt_dot(a, b):
    return lax.dot_general(a, b, (((1,), (1,)), ((), ())), preferred_element_type=jnp.float32)


def tn_dot(a, b):
    return lax.dot_general(a, b, (((0,), (0,)), ((), ())), preferred_element_type=jnp.float32)


def mixer_kernel(
    sp_size,
    tp_size,
    q_ref,
    f_ref,
    v_ref,
    g_ref,
    fmin_ref,
    extra_ref,
    gain_ref,
    wo_ref,
    stream_ref,
    ffgain_ref,
    residual_ref,
    normed_ref,
    local_ref,
    qtot_ref,
    incl_ref,
    incl_dec_ref,
    excl_ref,
    excl_dec_ref,
    st_send,
    st_recv,
    hid_ref,
    acc_ref,
    proj_ref,
    cols_ref,
    st_send_sem,
    st_recv_sem,
    hid_send_sem,
    hid_recv_sem,
    col_send_sem,
    col_recv_sem,
):
    sp_me, tp_me = lax.axis_index("sp"), lax.axis_index("tp")
    rows, width = q_ref.shape
    lanes = STATE_ROW_COUNT
    heads = width // lanes
    spans = rows // SPAN
    state_rows = heads * lanes
    distances = []
    while (1 << len(distances)) < sp_size:
        distances.append(1 << len(distances))

    barrier = pltpu.get_barrier_semaphore()
    expected = tp_size - 1
    for d in distances:
        has_next = sp_me + d < sp_size
        has_prev = sp_me >= d
        expected = expected + has_next.astype(jnp.int32) + has_prev.astype(jnp.int32)

        @pl.when(has_next)
        def _():
            pl.semaphore_signal(
                barrier, inc=1, device_id=(sp_me + d, tp_me), device_id_type=MESH
            )

        @pl.when(has_prev)
        def _():
            pl.semaphore_signal(
                barrier, inc=1, device_id=(sp_me - d, tp_me), device_id_type=MESH
            )

    for o in range(1, tp_size):
        pl.semaphore_signal(
            barrier,
            inc=1,
            device_id=(sp_me, lax.rem(tp_me + o, tp_size)),
            device_id_type=MESH,
        )

    causal = lax.broadcasted_iota(jnp.int32, (SPAN, SPAN), 0) >= lax.broadcasted_iota(
        jnp.int32, (SPAN, SPAN), 1
    )
    ones_low = jnp.where(causal, 1.0, 0.0).astype(jnp.float32)
    incl_dec_ref[...] = jnp.zeros_like(incl_dec_ref)
    for h in range(heads):
        cols = slice(h * lanes, (h + 1) * lanes)
        state = jnp.zeros((lanes, lanes), jnp.float32)
        base = jnp.zeros((1, lanes), jnp.float32)
        floor_gap = 1.0 - fmin_ref[:, cols]
        for c in range(spans):
            at = slice(c * SPAN, (c + 1) * SPAN)
            query = silu(q_ref[at, cols].astype(jnp.float32))
            weight = floor_gap / (1.0 + jnp.exp(f_ref[at, cols].astype(jnp.float32)))
            log_decay = jnp.log(1.0 - weight) + extra_ref[at, h : h + 1]
            running = jnp.dot(
                ones_low,
                log_decay,
                precision=lax.Precision.HIGHEST,
                preferred_element_type=jnp.float32,
            )
            final = running[SPAN - 1 : SPAN, :]
            value = v_ref[at, cols]
            q_dec = query * jnp.exp(running)
            q_low = q_dec.astype(jnp.bfloat16)
            k_low = (weight * jnp.exp(-running)).astype(jnp.bfloat16)
            k_end = (weight * jnp.exp(final - running)).astype(jnp.bfloat16)
            scores = jnp.where(causal, nt_dot(q_low, k_low), 0.0).astype(jnp.bfloat16)
            out = jnp.dot(scores, value, preferred_element_type=jnp.float32)
            if c:
                out = out + nt_dot(q_low, state.astype(jnp.bfloat16))
            local_ref[at, cols] = out
            qtot_ref[at, cols] = (q_dec * jnp.exp(base)).astype(jnp.bfloat16)
            state = jnp.exp(final) * state + tn_dot(value, k_end)
            base = base + final
        incl_ref[h * lanes : (h + 1) * lanes, :] = state
        incl_dec_ref[h : h + 1, :] = base

    excl_ref[...] = jnp.zeros_like(excl_ref)
    excl_dec_ref[...] = jnp.zeros_like(excl_dec_ref)
    pl.semaphore_wait(barrier, expected)

    def state_copy(r):
        return pltpu.make_async_remote_copy(
            src_ref=st_send.at[r],
            dst_ref=st_recv.at[r],
            send_sem=st_send_sem.at[r],
            recv_sem=st_recv_sem.at[r],
            device_id=(lax.rem(sp_me + distances[r], sp_size), tp_me),
            device_id_type=MESH,
        )

    for r, d in enumerate(distances):
        st_send[r, :state_rows, :] = incl_ref[...].astype(jnp.bfloat16)
        st_send[r, state_rows:, :] = incl_dec_ref[...].astype(jnp.bfloat16)

        @pl.when(sp_me + d < sp_size)
        def _():
            state_copy(r).start()

        @pl.when(sp_me >= d)
        def _():
            state_copy(r).wait_recv()
            earlier_dec = st_recv[r, state_rows:, :].astype(jnp.float32)
            for h in range(heads):
                at = slice(h * lanes, (h + 1) * lanes)
                earlier = st_recv[r, at, :].astype(jnp.float32)
                excl_ref[at, :] = excl_ref[at, :] + earlier * jnp.exp(excl_dec_ref[h : h + 1, :])
                if d != distances[-1]:
                    incl_ref[at, :] = incl_ref[at, :] + earlier * jnp.exp(
                        incl_dec_ref[h : h + 1, :]
                    )
            excl_dec_ref[...] = excl_dec_ref[...] + earlier_dec
            incl_dec_ref[...] = incl_dec_ref[...] + earlier_dec

    for h in range(heads):
        cols = slice(h * lanes, (h + 1) * lanes)
        carried = excl_ref[cols, :].astype(jnp.bfloat16)
        mixed = local_ref[:, cols] + nt_dot(qtot_ref[:, cols], carried)
        mean = jnp.mean(mixed * mixed, axis=-1, keepdims=True)
        normalized = mixed * lax.rsqrt(mean + epsilon)
        gated = normalized * gain_ref[:, cols] * silu(g_ref[:, cols].astype(jnp.float32))
        hid_ref[tp_me, :, cols] = gated.astype(jnp.bfloat16)

    def hidden_copy(o, source):
        return pltpu.make_async_remote_copy(
            src_ref=hid_ref.at[source],
            dst_ref=hid_ref.at[source],
            send_sem=hid_send_sem.at[o],
            recv_sem=hid_recv_sem.at[o],
            device_id=(sp_me, lax.rem(tp_me + o, tp_size)),
            device_id_type=MESH,
        )

    for o in range(1, tp_size):
        hidden_copy(o, tp_me).start()

    def part(source):
        at = pl.ds(pl.multiple_of(source * width, width), width)
        return jnp.dot(hid_ref[source], wo_ref[at, :], preferred_element_type=jnp.float32)

    acc_ref[...] = part(tp_me)
    for o in range(1, tp_size):
        source = lax.rem(tp_me + tp_size - o, tp_size)
        hidden_copy(o, source).wait_recv()
        acc_ref[...] += part(source)
    own_rows = residual_ref.shape[0]
    for p in range(tp_size):
        proj_ref[p] = acc_ref[p * own_rows : (p + 1) * own_rows, :].astype(jnp.bfloat16)

    def column_copy(o, source):
        return pltpu.make_async_remote_copy(
            src_ref=proj_ref.at[lax.rem(tp_me + o, tp_size)],
            dst_ref=cols_ref.at[source],
            send_sem=col_send_sem.at[o],
            recv_sem=col_recv_sem.at[o],
            device_id=(sp_me, lax.rem(tp_me + o, tp_size)),
            device_id_type=MESH,
        )

    for o in range(1, tp_size):
        column_copy(o, tp_me).start()
    cols_ref[tp_me] = proj_ref[tp_me]
    for o in range(1, tp_size):
        column_copy(o, lax.rem(tp_me + tp_size - o, tp_size)).wait_recv()
    part_width = cols_ref.shape[2]
    squares = jnp.zeros((own_rows, 1), jnp.float32)
    for p in range(tp_size):
        cols = slice(p * part_width, (p + 1) * part_width)
        residual = stream_ref[:, cols].astype(jnp.float32) + cols_ref[p].astype(jnp.float32)
        residual_ref[:, cols] = residual
        squares = squares + jnp.sum(residual * residual, axis=-1, keepdims=True)
    scale = lax.rsqrt(squares / (part_width * tp_size) + epsilon)
    normed_ref[...] = (residual_ref[...] * scale * ffgain_ref[...]).astype(jnp.bfloat16)

    for r, d in enumerate(distances):

        @pl.when(sp_me + d < sp_size)
        def _():
            state_copy(r).wait_send()

    for o in range(1, tp_size):
        hidden_copy(o, tp_me).wait_send()
        column_copy(o, tp_me).wait_send()


def mixer(
    query,
    forget_preact,
    value_input,
    output_gate,
    forget_minimum,
    extra_log_decay,
    head_norm_gain,
    output_weight,
    stream,
    feedforward_gain,
):
    sp_size, tp_size = lax.axis_size("sp"), lax.axis_size("tp")
    rows, width = query.shape
    heads = width // STATE_ROW_COUNT
    own_rows, model_width = stream.shape
    rounds = max(1, (sp_size - 1).bit_length())
    state_rows = heads * STATE_ROW_COUNT
    dec_rows = -(-heads // 16) * 16
    lanes = VALUE_CHANNELS
    columns = output_weight.shape[1]
    vmem = pl.BlockSpec(memory_space=pltpu.VMEM)
    dma = pltpu.SemaphoreType.DMA
    return pl.pallas_call(
        functools.partial(mixer_kernel, sp_size, tp_size),
        out_shape=(
            jax.ShapeDtypeStruct((own_rows, model_width), jnp.float32),
            jax.ShapeDtypeStruct((own_rows, model_width), jnp.bfloat16),
        ),
        in_specs=[vmem] * 10,
        out_specs=(vmem, vmem),
        scratch_shapes=[
            pltpu.VMEM((rows, width), jnp.float32),
            pltpu.VMEM((rows, width), jnp.bfloat16),
            pltpu.VMEM((state_rows, lanes), jnp.float32),
            pltpu.VMEM((dec_rows, lanes), jnp.float32),
            pltpu.VMEM((state_rows, lanes), jnp.float32),
            pltpu.VMEM((dec_rows, lanes), jnp.float32),
            pltpu.VMEM((rounds, state_rows + dec_rows, lanes), jnp.bfloat16),
            pltpu.VMEM((rounds, state_rows + dec_rows, lanes), jnp.bfloat16),
            pltpu.VMEM((tp_size, rows, width), jnp.bfloat16),
            pltpu.VMEM((rows, columns), jnp.float32),
            pltpu.VMEM((tp_size, own_rows, columns), jnp.bfloat16),
            pltpu.VMEM((tp_size, own_rows, columns), jnp.bfloat16),
            dma((rounds,)),
            dma((rounds,)),
            dma((tp_size,)),
            dma((tp_size,)),
            dma((tp_size,)),
            dma((tp_size,)),
        ],
        compiler_params=pltpu.CompilerParams(collective_id=0, has_side_effects=True),
        cost_estimate=pl.CostEstimate(
            flops=2 * rows * width * tp_size * columns,
            bytes_accessed=2 * (output_weight.size + 8 * query.size),
            transcendentals=6 * query.size,
        ),
        name="mixer",
    )(
        query,
        forget_preact,
        value_input,
        output_gate,
        forget_minimum[None],
        jnp.transpose(extra_log_decay),
        head_norm_gain[None],
        output_weight,
        stream,
        feedforward_gain[None],
    )


def flip(index, step, size):
    out = index
    bit = 1
    while bit < size:
        out = out + bit * (lax.rem(lax.div(step, bit), 2)) * (1 - 2 * lax.rem(lax.div(index, bit), 2))
        bit *= 2
    return out


def experts_kernel(
    sp_size,
    tp_size,
    cap,
    normed_ref,
    residual_ref,
    routes_ref,
    score_ref,
    gate_hbm,
    up_hbm,
    down_hbm,
    out_ref,
    table_ref,
    weight_ref,
    gu_ref,
    down_ref,
    send_ref,
    rows_ref,
    part_ref,
    part_in,
    own_ref,
    xsum_ref,
    xsum_in,
    back_ref,
    result_ref,
    load_sem,
    go_send,
    go_recv,
    sib_send,
    sib_recv,
    x_send,
    x_recv,
    relay_send,
    relay_recv,
    part_send,
    part_recv,
    xsum_send,
    xsum_recv,
    back_send,
    back_recv,
):
    sp_me, tp_me = lax.axis_index("sp"), lax.axis_index("tp")
    tokens, width = normed_ref.shape
    hidden = down_ref.shape[0]
    slots = sp_size * cap
    sibling = tp_me + 1 - 2 * lax.rem(tp_me, 2)
    across = lax.rem(tp_me + tp_size // 2, tp_size)

    loads = [
        pltpu.make_async_copy(gate_hbm.at[0], gu_ref.at[:, pl.ds(0, hidden)], load_sem.at[0]),
        pltpu.make_async_copy(up_hbm.at[0], gu_ref.at[:, pl.ds(hidden, hidden)], load_sem.at[1]),
        pltpu.make_async_copy(down_hbm.at[0], down_ref, load_sem.at[2]),
    ]
    for load in loads:
        load.start()

    barrier = pltpu.get_barrier_semaphore()
    for k in range(1, sp_size):
        pl.semaphore_signal(
            barrier, inc=1, device_id=(flip(sp_me, k, sp_size), tp_me), device_id_type=MESH
        )
    for peer in (sibling, across):
        pl.semaphore_signal(barrier, inc=1, device_id=(sp_me, peer), device_id_type=MESH)

    own_routes = routes_ref[pl.ds(pl.multiple_of(tp_me * tokens, tokens), tokens), :]
    lane = lax.broadcasted_iota(jnp.int32, (1, slots), 1)
    step_of = lane // cap
    expert = jnp.zeros((1, slots), jnp.int32)
    bit = 1
    while bit < sp_size:
        mine = lax.rem(lax.div(sp_me, bit), 2)
        theirs = (step_of // bit) % 2
        expert = expert + bit * (theirs + mine - 2 * theirs * mine)
        bit *= 2
    first = own_routes[:, 0:1] == expert
    second = own_routes[:, 1:2] == expert
    named = jnp.where(first | second, 1.0, 0.0)
    earlier = jnp.where(
        lax.broadcasted_iota(jnp.int32, (tokens, tokens), 0)
        > lax.broadcasted_iota(jnp.int32, (tokens, tokens), 1),
        1.0,
        0.0,
    )
    rank = jnp.dot(
        earlier.astype(jnp.bfloat16),
        named.astype(jnp.bfloat16),
        preferred_element_type=jnp.float32,
    )
    hit = jnp.where(rank == (lane % cap).astype(jnp.float32), named, 0.0)
    table_ref[...] = hit.astype(jnp.bfloat16)
    score = score_ref[...]
    share = score / jnp.sum(score, axis=1, keepdims=True)
    weight = hit * jnp.where(first, share[:, 0:1], share[:, 1:2])
    high = weight.astype(jnp.bfloat16)
    weight_ref[:tokens, :] = high
    weight_ref[tokens:, :] = (weight - high.astype(jnp.float32)).astype(jnp.bfloat16)

    pl.semaphore_wait(barrier, sp_size + 1)

    def go_copy(k):
        return pltpu.make_async_remote_copy(
            src_ref=send_ref.at[k],
            dst_ref=rows_ref.at[k, 0],
            send_sem=go_send.at[k],
            recv_sem=go_recv.at[k],
            device_id=(flip(sp_me, k, sp_size), tp_me),
            device_id_type=MESH,
        )

    def tp_copy(src, dst, send_sem, recv_sem, peer):
        return pltpu.make_async_remote_copy(
            src_ref=src,
            dst_ref=dst,
            send_sem=send_sem,
            recv_sem=recv_sem,
            device_id=(sp_me, peer),
            device_id_type=MESH,
        )

    def sib_copy(k):
        return tp_copy(
            rows_ref.at[k, 0], rows_ref.at[k, 1], sib_send.at[k], sib_recv.at[k], sibling
        )

    def x_copy(k):
        return tp_copy(rows_ref.at[k, 0], rows_ref.at[k, 2], x_send.at[k], x_recv.at[k], across)

    def relay_copy(k):
        return tp_copy(
            rows_ref.at[k, 2], rows_ref.at[k, 3], relay_send.at[k], relay_recv.at[k], sibling
        )

    def part_copy(k):
        return tp_copy(
            part_ref.at[k], part_in.at[k], part_send.at[k], part_recv.at[k], sibling
        )

    def xsum_copy(k):
        return tp_copy(xsum_ref.at[k], xsum_in.at[k], xsum_send.at[k], xsum_recv.at[k], across)

    def back_copy(k):
        return pltpu.make_async_remote_copy(
            src_ref=back_ref.at[k],
            dst_ref=result_ref.at[k],
            send_sem=back_send.at[k],
            recv_sem=back_recv.at[k],
            device_id=(flip(sp_me, k, sp_size), tp_me),
            device_id_type=MESH,
        )

    group = max(1, min(sp_size, 128 // cap))
    for first_k in range(0, sp_size, group):
        picked = tn_dot(
            table_ref[:, first_k * cap : (first_k + group) * cap], normed_ref[...]
        ).astype(jnp.bfloat16)
        for k in range(first_k, first_k + group):
            block = picked[(k - first_k) * cap : (k - first_k + 1) * cap, :]
            if k:
                send_ref[k] = block
                go_copy(k).start()
            else:
                rows_ref[0, 0] = block

    def compute(k):
        x = rows_ref[k].reshape(4 * cap, width)
        both = jnp.dot(x, gu_ref[...], preferred_element_type=jnp.float32)
        inner = (silu(both[:, :hidden]) * both[:, hidden:]).astype(jnp.bfloat16)
        tile = width // 3 if width % 384 == 0 else width
        for c in range(width // tile):
            cols = slice(c * tile, (c + 1) * tile)
            part = jnp.dot(inner, down_ref[:, cols], preferred_element_type=jnp.float32)
            part_ref[k, 0, :, cols] = part[cap : 2 * cap].astype(jnp.bfloat16)
            part_ref[k, 1, :, cols] = part[3 * cap :].astype(jnp.bfloat16)
            own_ref[k, 0, :, cols] = part[:cap]
            own_ref[k, 1, :, cols] = part[2 * cap : 3 * cap]

    def body(i, carry):
        @pl.when(i < sp_size)
        def _():
            @pl.when(i > 0)
            def _():
                go_copy(i).wait_recv()

            x_copy(i).start()
            sib_copy(i).start()

        @pl.when((i >= 1) & (i < sp_size + 1))
        def _():
            k = i - 1
            x_copy(k).wait_recv()
            relay_copy(k).start()

        @pl.when((i >= 3) & (i < sp_size + 3))
        def _():
            k = i - 3
            part_copy(k).wait_recv()
            xsum_ref[k] = (own_ref[k, 1] + part_in[k, 1].astype(jnp.float32)).astype(jnp.bfloat16)
            xsum_copy(k).start()

        @pl.when((i >= 2) & (i < sp_size + 2))
        def _():
            k = i - 2

            @pl.when(k == 0)
            def _():
                for load in loads:
                    load.wait()

            sib_copy(k).wait_recv()
            relay_copy(k).wait_recv()
            compute(k)
            part_copy(k).start()

        @pl.when(i >= 4)
        def _():
            k = i - 4
            xsum_copy(k).wait_recv()
            final = (
                own_ref[k, 0]
                + part_in[k, 0].astype(jnp.float32)
                + xsum_in[k].astype(jnp.float32)
            ).astype(jnp.bfloat16)

            @pl.when(k > 0)
            def _():
                back_ref[k] = final
                back_copy(k).start()

            @pl.when(k == 0)
            def _():
                result_ref[0] = final

        return carry

    lax.fori_loop(0, sp_size + 4, body, 0)

    half = sp_size // 2
    tile = width // 3 if width % 384 == 0 else width
    for part in range(2):
        for k in range(part * half, (part + 1) * half):
            if k:
                back_copy(k).wait_recv()
        for c in range(width // tile):
            cols = slice(c * tile, (c + 1) * tile)
            rows = result_ref[part * half : (part + 1) * half, :, cols].reshape(half * cap, tile)
            sums = jnp.dot(
                weight_ref[:, part * half * cap : (part + 1) * half * cap],
                rows,
                preferred_element_type=jnp.float32,
            )
            total = sums[:tokens] + sums[tokens:] + residual_ref[:, cols]
            if part:
                out_ref[:, cols] = (total + own_ref[0, :, :, cols].reshape(2 * cap, tile)).astype(
                    jnp.bfloat16
                )
            else:
                own_ref[0, :, :, cols] = (sums[:tokens] + sums[tokens:]).reshape(2, cap, tile)

    for k in range(sp_size):
        if k:
            go_copy(k).wait_send()
            back_copy(k).wait_send()
        sib_copy(k).wait_send()
        x_copy(k).wait_send()
        relay_copy(k).wait_send()
        part_copy(k).wait_send()
        xsum_copy(k).wait_send()


def experts(normed, residual, routes, router_weight, gate, up, down):
    sp_size, tp_size = lax.axis_size("sp"), lax.axis_size("tp")
    tokens, width = normed.shape
    cap = routes.shape[0] // sp_size
    hidden = gate.shape[2]
    slots = sp_size * cap
    vmem = pl.BlockSpec(memory_space=pltpu.VMEM)
    hbm = pl.BlockSpec(memory_space=pl.ANY)
    dma = pltpu.SemaphoreType.DMA
    low = jnp.bfloat16
    return pl.pallas_call(
        functools.partial(experts_kernel, sp_size, tp_size, cap),
        out_shape=jax.ShapeDtypeStruct((tokens, width), low),
        in_specs=[vmem] * 4 + [hbm] * 3,
        out_specs=vmem,
        scratch_shapes=[
            pltpu.VMEM((tokens, slots), low),
            pltpu.VMEM((2 * tokens, slots), low),
            pltpu.VMEM((width, 2 * hidden), low),
            pltpu.VMEM((hidden, width), low),
            pltpu.VMEM((sp_size, cap, width), low),
            pltpu.VMEM((sp_size, 4, cap, width), low),
            pltpu.VMEM((sp_size, 2, cap, width), low),
            pltpu.VMEM((sp_size, 2, cap, width), low),
            pltpu.VMEM((sp_size, 2, cap, width), jnp.float32),
            pltpu.VMEM((sp_size, cap, width), low),
            pltpu.VMEM((sp_size, cap, width), low),
            pltpu.VMEM((sp_size, cap, width), low),
            pltpu.VMEM((sp_size, cap, width), low),
            dma((3,)),
        ]
        + [dma((sp_size,))] * 14,
        compiler_params=pltpu.CompilerParams(collective_id=1, has_side_effects=True),
        cost_estimate=pl.CostEstimate(
            flops=6 * 4 * slots * width * hidden,
            bytes_accessed=6 * width * hidden,
            transcendentals=4 * slots * hidden,
        ),
        name="experts",
    )(normed, residual, routes, router_weight, gate, up, down)


def dispatch_table(slot_ids, window_rows, quarter_rows):
    groups = slot_ids.shape[0]
    slot_grid = lax.broadcasted_iota(jnp.int32, (groups, window_rows, slot_ids.shape[1]), 1)
    hits = (slot_grid == slot_ids[:, None, :]).astype(jnp.bfloat16)
    return jnp.sum(hits.reshape(groups, window_rows, quarter_rows, TOPK), axis=3)


def small_enough(sp_size, tp_size, capacity, tokens):
    return (
        tp_size == 4
        and sp_size <= 16
        and sp_size & (sp_size - 1) == 0
        and capacity % 16 == 0
        and tokens == 2 * capacity
    )


def per_device(
    query,
    forget_preact,
    value_input,
    output_gate,
    forget_minimum,
    extra_log_decay,
    head_norm_gain,
    output_weight,
    stream,
    feedforward_gain,
    routes,
    router_weight,
    expert_gate_weight,
    expert_up_weight,
    expert_down_weight,
):
    window_rows = query.shape[0]
    tp_size = lax.axis_size("tp")
    sp_size = lax.axis_size("sp")
    residual, normed = mixer(
        query,
        forget_preact,
        value_input,
        output_gate,
        forget_minimum,
        extra_log_decay,
        head_norm_gain,
        output_weight,
        stream,
        feedforward_gain,
    )
    quarter_rows = stream.shape[0]
    capacity = window_rows // sp_size
    if small_enough(sp_size, tp_size, capacity, quarter_rows):
        return experts(
            normed,
            residual,
            routes,
            router_weight,
            expert_gate_weight,
            expert_up_weight,
            expert_down_weight,
        )
    gate_all = lax.all_gather(expert_gate_weight[0], "tp")
    up_all = lax.all_gather(expert_up_weight[0], "tp")
    down_all = lax.all_gather(expert_down_weight[0], "tp")
    pick_ids = routes.reshape(tp_size, quarter_rows * TOPK)
    onehot = (pick_ids[:, :, None] == jnp.arange(sp_size, dtype=jnp.int32)[None, None, :]).astype(
        jnp.int32
    )
    rank_ids = jnp.sum((jnp.cumsum(onehot, axis=1) - 1) * onehot, axis=2)
    slot_ids = pick_ids * capacity + rank_ids
    own_index = lax.axis_index("tp")
    own_slots = lax.dynamic_slice_in_dim(slot_ids, own_index, 1, 0)
    send_table = dispatch_table(own_slots, window_rows, quarter_rows)[0]
    sendbuf = jnp.dot(send_table, normed, preferred_element_type=jnp.float32).astype(jnp.bfloat16)
    received = lax.all_to_all(
        sendbuf.reshape(sp_size, capacity, -1), "sp", split_axis=0, concat_axis=0, tiled=True
    )
    flat_rows = received.reshape(window_rows, -1)
    gate_act = jnp.einsum("nd,tdf->tnf", flat_rows, gate_all, preferred_element_type=jnp.float32)
    up_act = jnp.einsum("nd,tdf->tnf", flat_rows, up_all, preferred_element_type=jnp.float32)
    inner_act = (jax.nn.silu(gate_act) * up_act).astype(jnp.bfloat16)
    inner_all = jnp.transpose(inner_act, (1, 0, 2)).reshape(window_rows, -1)
    down_flat = down_all.reshape(-1, down_all.shape[-1])
    expert_out = jnp.dot(inner_all, down_flat, preferred_element_type=jnp.float32).astype(
        jnp.bfloat16
    )
    returned = lax.all_to_all(
        expert_out.reshape(sp_size, capacity, -1), "sp", split_axis=0, concat_axis=0, tiled=True
    )
    results = returned.reshape(window_rows, -1)
    route_weight = router_weight / jnp.sum(router_weight, axis=1, keepdims=True)
    row_slots = own_slots.reshape(quarter_rows, TOPK)
    slot_grid = lax.broadcasted_iota(jnp.int32, (quarter_rows, TOPK, window_rows), 2)
    table = jnp.sum(
        jnp.where(slot_grid == row_slots[:, :, None], route_weight[:, :, None], 0.0), axis=1
    )
    table_high = table.astype(jnp.bfloat16)
    table_low = (table - table_high.astype(jnp.float32)).astype(jnp.bfloat16)
    routed_sum = jnp.dot(table_high, results, preferred_element_type=jnp.float32) + jnp.dot(
        table_low, results, preferred_element_type=jnp.float32
    )
    return (residual + routed_sum).astype(jnp.bfloat16)


def solution(mesh):
    placed = (
        P("sp", "tp"),
        P("sp", "tp"),
        P("sp", "tp"),
        P("sp", "tp"),
        P("tp"),
        P("tp", "sp"),
        P("tp"),
        P(None, "tp"),
        P(("sp", "tp"), None),
        P(),
        P("sp", None),
        P(("sp", "tp"), None),
        P("sp", None, "tp"),
        P("sp", None, "tp"),
        P("sp", "tp", None),
    )
    return jax.shard_map(
        per_device, mesh=mesh, in_specs=placed, out_specs=P(("sp", "tp"), None), check_vma=False
    )
```
